32 devices in a mesh: sp: 4 (over y, x), tp: 8 (over z, core).
Axes of the slice: x: 2, y: 2, z: 4, core: 2. Of those that a mesh axis runs over, the one named last changes fastest.
Arguments:
- stream: bfloat16 [8, 1536, 2048], P('tp', 'sp'), may hold values from -80 to 80
- norm_gain: float32 [2048], replicated, may hold values from 0.1 to 1.9
- w_lin: bfloat16 [1024, 2048], P('tp'), may hold values from -0.125 to 0.125
- w_gate: bfloat16 [1024, 2048], P('tp'), may hold values from -0.125 to 0.125
- conv_taps: bfloat16 [31, 1024], replicated, may hold values from -3 to 3
- conv_bias: float32 [1024], replicated, may hold values from -3 to 3
- ln_gain: float32 [1024], replicated, may hold values from 0.1 to 1.9
- ln_shift: float32 [1024], replicated, may hold values from -3 to 3
- w_proj: bfloat16 [1024, 2048], P('tp'), may hold values from -0.1875 to 0.1875
Outputs:
- result_stream: bfloat16 [8, 1536, 2048], P('tp', 'sp')
The draws below stay inside these ranges and needn't reach their ends.
All inputs are finite; a program needn't handle non-finite values.
Results may differ from the reference program's by a relative error of at most 0.0024.
Values may be sent and summed in bfloat16 or wider, within the bound.
No kernel may reach another device: no remote copies, remote signals or barrier semaphores. Data moves between devices by JAX's collectives and lax.ppermute only.
A program may use at most 64 MiB of HBM per device.

```python
import jax
import jax.numpy as jnp
from jax import lax

D = 2048
CC = 1024
KW = 31
SEQ_LEN = 1536
SEQS = 8


def draw_stream(key, part):
    k_base, k_cols, k_rows = jax.random.split(jax.random.fold_in(key, 11), 3)
    cols = jnp.arange(D, dtype=jnp.float32) / D
    col_scale = jnp.exp(jnp.log(4.0) * cols) * jnp.exp(jax.random.uniform(k_cols, (D,), jnp.float32, -0.35, 0.35))
    row_scale = jnp.exp(jax.random.uniform(k_rows, (SEQS, SEQ_LEN, 1), jnp.float32, 0.0, jnp.log(10.0))) / 3.0
    base = jnp.clip(jax.random.normal(k_base, (SEQS, SEQ_LEN, D), jnp.float32), -4.0, 4.0)
    return (base * row_scale * col_scale).astype(jnp.bfloat16)


def draw_conv_taps(key, part):
    k_base, k_cols = jax.random.split(jax.random.fold_in(key, 23), 2)
    cols = jnp.arange(CC, dtype=jnp.float32) / CC
    col_scale = jnp.exp(jnp.log(3.0) * cols) * jnp.exp(jax.random.uniform(k_cols, (1, CC), jnp.float32, -0.35, 0.35))
    base = jnp.clip(jax.random.normal(k_base, (KW, CC), jnp.float32), -3.5, 3.5)
    return (base * col_scale * KW ** (-0.5)).astype(jnp.bfloat16)


def level_of(stream_key, dims, pieces, smallest, top_value):
    loudness = 1.0
    for dim, shards_of in pieces:
        draws = jax.random.uniform(jax.random.fold_in(jax.random.fold_in(stream_key, 6), dim), (shards_of,), jnp.float32, smallest / len(pieces), top_value / len(pieces))
        loudness = loudness * jnp.repeat(jnp.exp(draws), dims[dim] // shards_of).reshape((-1,) + (1,) * (len(dims) - 1 - dim))
    return loudness


def gaussian(key, shape, deviation, reach, cuts=(), kind=jnp.bfloat16):
    drawn = deviation * jax.random.normal(key, shape, jnp.float32)
    if cuts:
        drawn = drawn * level_of(key, shape, cuts, -0.22, 0.18)
    return jnp.clip(drawn, -reach, reach).astype(kind)


def setup_inputs(seed: int = 0) -> dict:
    seeds = jax.random.split(jax.random.key(seed), 10)
    return {
        "stream": draw_stream(jax.random.fold_in(seeds[9], 71), 0),
        "norm_gain": jnp.clip(1.0 + 0.18 * jax.random.normal(seeds[1], (D,), jnp.float32), 0.1, 1.9),
        "w_lin": gaussian(seeds[2], (CC, D), D ** -0.5, 0.125, ((0, 8),)),
        "w_gate": gaussian(seeds[3], (CC, D), D ** -0.5, 0.125, ((0, 8),)),
        "conv_taps": draw_conv_taps(jax.random.fold_in(seeds[9], 71), 0),
        "conv_bias": gaussian(seeds[5], (CC,), 0.5, 3.0, (), jnp.float32),
        "ln_gain": jnp.clip(1.0 + 0.18 * jax.random.normal(seeds[6], (CC,), jnp.float32), 0.1, 1.9),
        "ln_shift": gaussian(seeds[7], (CC,), 0.5, 3.0, (), jnp.float32),
        "w_proj": gaussian(seeds[8], (CC, D), CC ** -0.5, 0.1875, ((0, 8),)),
    }


EPS = 1e-06

def rms_rows(rows, gain):
    full = rows.astype(jnp.float32)
    scale = lax.rsqrt(lax.optimization_barrier(jnp.mean(full * full, axis=1, keepdims=True)) + EPS)
    return (full * scale * gain.astype(jnp.float32)).astype(jnp.bfloat16)

def project_rows(normed, weight):
    return lax.dot_general(normed, weight, (((1,), (1,)), ((), ())), preferred_element_type=jnp.float32)

def reference(stream, norm_gain, w_lin, w_gate, conv_taps, conv_bias, ln_gain, ln_shift, w_proj):
    taps_full = conv_taps.astype(jnp.float32)

    def one_sequence(current):
        normed = rms_rows(current, norm_gain)
        linear = project_rows(normed, w_lin)
        gating = project_rows(normed, w_gate)
        mixed = (linear * jax.nn.sigmoid(gating)).astype(jnp.bfloat16)
        length = current.shape[0]
        padded = jnp.pad(mixed.astype(jnp.float32), ((KW - 1, 0), (0, 0)))
        conv = jnp.zeros((length, mixed.shape[1]), jnp.float32)
        for tap in range(KW):
            conv = conv + taps_full[tap] * padded[tap:tap + length]
        conv = conv + conv_bias
        mean = lax.optimization_barrier(jnp.mean(conv, axis=1, keepdims=True))
        meansq = lax.optimization_barrier(jnp.mean(conv * conv, axis=1, keepdims=True))
        var = meansq - mean * mean
        activated = jax.nn.silu((conv - mean) * lax.rsqrt(var + EPS) * ln_gain + ln_shift).astype(jnp.bfloat16)
        projected = jnp.dot(activated, w_proj, preferred_element_type=jnp.float32)
        return (current.astype(jnp.float32) + projected).astype(jnp.bfloat16)
    return lax.map(one_sequence, stream)
```

```python
import functools

import jax
import jax.numpy as jnp
from jax import lax
from jax.experimental import pallas as pl
from jax.experimental.pallas import tpu as pltpu
from jax.sharding import PartitionSpec as P

KW = 31
REACH = KW - 1
HALO = 32
EPS = 1e-06
F32 = jnp.float32
BF16 = jnp.bfloat16
VMEM = pl.BlockSpec(memory_space=pltpu.VMEM)


def rms_rows(rows, gain):
    full = rows.astype(F32)
    scale = lax.rsqrt(jnp.mean(full * full, axis=1, keepdims=True) + EPS)
    return (full * scale * gain).astype(BF16)


def passed_along(value, axis, steps):
    count = lax.axis_size(axis)
    leading, last = (max(0, -steps), min(count, count - steps))
    return lax.ppermute(value, axis, [(source, source + steps) for source in range(leading, last)])


def plain(stream, norm_gain, w_lin, w_gate, conv_taps, conv_bias, ln_gain, ln_shift, w_proj):
    rows = stream.shape[1]
    current = stream[0]
    normed = rms_rows(current, norm_gain)
    paired = jnp.stack([w_lin, w_gate], axis=1)
    both = jnp.einsum(
        "td,nrd->trn",
        normed,
        lax.all_gather(paired, "tp", axis=0, tiled=True),
        preferred_element_type=F32,
    )
    mixed = (both[:, 0] * jax.nn.sigmoid(both[:, 1])).astype(BF16)
    earlier_mixed = passed_along(mixed[rows - REACH :], "sp", 1)
    padded = jnp.concatenate([earlier_mixed, mixed], axis=0).astype(F32)
    taps_full = conv_taps.astype(F32)
    conv = jnp.zeros((rows, mixed.shape[1]), F32)
    for tap in range(KW):
        conv = conv + taps_full[tap] * padded[tap : tap + rows]
    conv = conv + conv_bias
    mean = jnp.mean(conv, axis=1, keepdims=True)
    meansq = jnp.mean(conv * conv, axis=1, keepdims=True)
    var = meansq - mean * mean
    activated = jax.nn.silu((conv - mean) * lax.rsqrt(var + EPS) * ln_gain + ln_shift).astype(BF16)
    projected = jnp.dot(
        activated, lax.all_gather(w_proj, "tp", axis=0, tiled=True), preferred_element_type=F32
    )
    return (current.astype(F32) + projected).astype(BF16)[None]


def piece_kernel(normed, mine, other, taps, bias, conv, mixed):
    rows, lanes = conv.shape
    half = lanes // 2
    hidden = normed[...]
    contract = (((1,), (1,)), ((), ()))
    for side, weights in enumerate((mine, other)):
        linear = lax.dot_general(hidden, weights[0], contract, preferred_element_type=F32)
        gating = lax.dot_general(hidden, weights[1], contract, preferred_element_type=F32)
        gated = (linear * jax.nn.sigmoid(gating)).astype(BF16)
        mixed[:, side * half : (side + 1) * half] = gated.astype(F32)
    block = 64
    for lane in range(0, lanes, 128):
        cols = pl.ds(lane, 128)
        for row in range(0, rows, block):
            total = jnp.broadcast_to(bias[0:1, cols], (block, 128))
            for low in range(8):
                reach = block + 24
                first = row + low + HALO - REACH
                reach = min(reach, mixed.shape[0] - first)
                window = mixed[pl.ds(first, reach), cols]
                for high in range(4):
                    tap = 8 * high + low
                    if tap < KW:
                        total += taps[tap : tap + 1, cols] * window[8 * high : 8 * high + block]
            conv[pl.ds(row, block), cols] = total


def piece(normed, mine, other, taps, bias):
    rows = normed.shape[0] - HALO
    lanes = 2 * mine.shape[1]
    flops = 4 * normed.shape[0] * normed.shape[1] * lanes
    return pl.pallas_call(
        piece_kernel,
        out_shape=jax.ShapeDtypeStruct((rows, lanes), F32),
        in_specs=[VMEM] * 5,
        out_specs=VMEM,
        scratch_shapes=[pltpu.VMEM((normed.shape[0], lanes), F32)],
        compiler_params=pltpu.CompilerParams(vmem_limit_bytes=24 * 2**20),
        cost_estimate=pl.CostEstimate(flops=flops, bytes_accessed=0, transcendentals=0),
    )(normed, mine, other, taps, bias)


def finish_kernel(count, current, gain, shift, *refs):
    convs, weights, out = refs[:count], refs[count:-1], refs[-1]
    lanes = convs[0].shape[1]
    channels = count * lanes
    total = sum(jnp.sum(c[...], axis=1, keepdims=True) for c in convs)
    square = sum(jnp.sum(c[...] * c[...], axis=1, keepdims=True) for c in convs)
    mean = total / channels
    var = square / channels - mean * mean
    scale = lax.rsqrt(var + EPS)
    projected = current[...].astype(F32)
    for k, c in enumerate(convs):
        y = (c[...] - mean) * scale * gain[k : k + 1] + shift[k : k + 1]
        act = (y * jax.nn.sigmoid(y)).astype(BF16)
        half = lanes // 2
        for side in range(2):
            projected += jnp.dot(
                act[:, side * half : (side + 1) * half], weights[2 * k + side][...], preferred_element_type=F32
            )
    out[...] = projected.astype(BF16)


def finish(current, gain, shift, convs, weights):
    rows, width = current.shape
    return pl.pallas_call(
        functools.partial(finish_kernel, len(convs)),
        out_shape=jax.ShapeDtypeStruct((rows, width), BF16),
        in_specs=[VMEM] * (3 + len(convs) + len(weights)),
        out_specs=VMEM,
        compiler_params=pltpu.CompilerParams(vmem_limit_bytes=32 * 2**20),
        cost_estimate=pl.CostEstimate(
            flops=2 * rows * width * len(convs) * convs[0].shape[1], bytes_accessed=0, transcendentals=0
        ),
    )(current, gain, shift, *convs, *weights)


def send(value, label, target):
    ways, both = lax.axis_size("sp"), lax.axis_size("tp")
    pairs = []
    for q in range(ways):
        for z in range(both // 2):
            for c in range(2):
                t = target(q, z, c)
                if t is not None:
                    pairs.append((q * both + z * 2 + c, t[0] * both + t[1] * 2 + t[2]))
    with jax.named_scope(label):
        return lax.ppermute(value, ("sp", "tp"), pairs)


def to_plane_first(q, z, c):
    return (q ^ (1 + c), z, c)


def to_plane_second(q, z, c):
    return (q ^ (2 - c), z, c)


def to_other_core(q, z, c):
    return (q, z, 1 - c)


def put(base, value, at):
    return lax.dynamic_update_slice_in_dim(base, value, at, 1)


def spread(value, label, q, c):
    r = value.shape[1]
    first, second = 1 + c, 2 - c
    p1 = send(value, "xa" + label, to_plane_first)
    two = jnp.concatenate([value, p1], axis=1)
    p2 = send(two, "xb" + label, to_plane_second)
    whole = jnp.zeros((value.shape[0], 4 * r, value.shape[2]), value.dtype)
    whole = put(whole, value, q * r)
    whole = put(whole, p1, (q ^ first) * r)
    whole = put(whole, p2[:, :r], (q ^ second) * r)
    return put(whole, p2[:, r:], (q ^ 3) * r)


def fast(stream, norm_gain, w_lin, w_gate, conv_taps, conv_bias, ln_gain, ln_shift, w_proj):
    current = stream[0]
    rows = current.shape[0]
    q, me = lax.axis_index("sp"), lax.axis_index("tp")
    z, c = me // 2, me % 2
    depth = lax.axis_size("tp") // 2
    shard = w_lin.shape[0]
    quarter = shard // lax.axis_size("sp")

    def cut(w):
        return lax.dynamic_slice_in_dim(w, q * quarter, quarter, 0)

    hops = [k for k in (1, 3, 2)]
    gates = jnp.stack([cut(w_lin), cut(w_gate)])
    far_gates = {k: send(gates, f"zg{k}", lambda q, z, c, k=k: (q, z ^ k, c)) for k in hops}
    ways = lax.axis_size("sp")
    earlier = send(current[rows - HALO :], "halo", lambda q, z, c: (q + 1, z, c) if q + 1 < ways else None)
    own_gates = jnp.stack([w_lin, w_gate])
    other_gates = send(own_gates, "dg0", to_other_core)
    other_proj = send(w_proj, "dp0", to_other_core)
    proj = cut(w_proj)
    far_proj = {k: send(proj, f"zp{k}", lambda q, z, c, k=k: (q, z ^ k, c)) for k in hops}

    normed = jnp.concatenate([rms_rows(earlier, norm_gain), rms_rows(current, norm_gain)], axis=0)

    def by_piece(p):
        p = p.astype(F32).reshape(-1, depth, 2 * shard)
        swapped = jnp.concatenate([p[:, :, shard:], p[:, :, :shard]], axis=2)
        return jnp.where(c == 0, p, swapped).transpose(1, 0, 2)

    taps = by_piece(conv_taps)
    small = by_piece(jnp.stack([conv_bias, ln_gain, ln_shift]))
    order = [0] + hops

    def of(p, k):
        return lax.dynamic_index_in_dim(p, z ^ k, 0, keepdims=False)

    params = [of(small, k) for k in order]
    convs = []
    for k, s in zip(order, params):
        if k == 0:
            mine, other = own_gates, other_gates
        else:
            mine = spread(far_gates[k], f"g{k}", q, c)
            other = send(mine, f"dg{k}", to_other_core)
        convs.append(piece(normed, mine, other, of(taps, k), s[0:1]))
    mine = spread(jnp.stack([far_proj[k] for k in hops]), "p", q, c)
    other = send(mine, "dp", to_other_core)
    weights = [w_proj, other_proj]
    for i in range(len(hops)):
        weights += [mine[i], other[i]]
    gain = jnp.concatenate([s[1:2] for s in params])
    shift = jnp.concatenate([s[2:3] for s in params])
    return finish(current, gain, shift, convs, weights)[None]


def local(mesh_shape, *args):
    shard = args[2].shape[0]
    ways, both = mesh_shape["sp"], mesh_shape["tp"]
    if ways == 4 and both == 8 and shard % (16 * ways) == 0 and shard % 128 == 0:
        return fast(*args)
    return plain(*args)


def solution(mesh):
    placed = (
        P("tp", "sp", None),
        P(),
        P("tp", None),
        P("tp", None),
        P(),
        P(),
        P(),
        P(),
        P("tp", None),
    )
    return jax.shard_map(
        functools.partial(local, dict(mesh.shape)),
        mesh=mesh,
        in_specs=placed,
        out_specs=P("tp", "sp", None),
        check_vma=False,
    )
```

```python
import functools

import jax
import jax.numpy as jnp
from jax import lax
from jax.experimental import pallas as pl
from jax.experimental.pallas import tpu as pltpu
from jax.sharding import PartitionSpec as P


KW = 31
REACH = KW - 1
HALO = 32
EPS = 1e-06
F32 = jnp.float32
BF16 = jnp.bfloat16
VMEM = pl.BlockSpec(memory_space=pltpu.VMEM)


def rms_rows(rows, gain):
    full = rows.astype(F32)
    scale = lax.rsqrt(jnp.mean(full * full, axis=1, keepdims=True) + EPS)
    return (full * scale * gain).astype(BF16)


def passed_along(value, axis, steps):
    count = lax.axis_size(axis)
    leading, last = (max(0, -steps), min(count, count - steps))
    return lax.ppermute(value, axis, [(source, source + steps) for source in range(leading, last)])


def plain(stream, norm_gain, w_lin, w_gate, conv_taps, conv_bias, ln_gain, ln_shift, w_proj):
    rows = stream.shape[1]
    current = stream[0]
    normed = rms_rows(current, norm_gain)
    paired = jnp.stack([w_lin, w_gate], axis=1)
    both = jnp.einsum(
        "td,nrd->trn",
        normed,
        lax.all_gather(paired, "tp", axis=0, tiled=True),
        preferred_element_type=F32,
    )
    mixed = (both[:, 0] * jax.nn.sigmoid(both[:, 1])).astype(BF16)
    earlier_mixed = passed_along(mixed[rows - REACH :], "sp", 1)
    padded = jnp.concatenate([earlier_mixed, mixed], axis=0).astype(F32)
    taps_full = conv_taps.astype(F32)
    conv = jnp.zeros((rows, mixed.shape[1]), F32)
    for tap in range(KW):
        conv = conv + taps_full[tap] * padded[tap : tap + rows]
    conv = conv + conv_bias
    mean = jnp.mean(conv, axis=1, keepdims=True)
    meansq = jnp.mean(conv * conv, axis=1, keepdims=True)
    var = meansq - mean * mean
    activated = jax.nn.silu((conv - mean) * lax.rsqrt(var + EPS) * ln_gain + ln_shift).astype(BF16)
    projected = jnp.dot(
        activated, lax.all_gather(w_proj, "tp", axis=0, tiled=True), preferred_element_type=F32
    )
    return (current.astype(F32) + projected).astype(BF16)[None]


def place():
    me = lax.axis_index("tp")
    return lax.axis_index("sp"), me // 2, me % 2


def aligned(value, unit):
    return pl.multiple_of(value * unit, unit)


HOPS = (0, 1, 3, 2)


def run_copies(pairs, sems):
    copies = [pltpu.make_async_copy(a, b, sems.at[i]) for i, (a, b) in enumerate(pairs)]
    for copy in copies:
        copy.start()
    for copy in copies:
        copy.wait()


def pack_kernel(join, *refs):
    parts, out = refs[:-1], refs[-1]
    step = parts[0].shape[-2]
    for i, part in enumerate(parts):
        if join:
            out[:, i * step : (i + 1) * step] = part[...]
        else:
            out[i] = part[...]


def pack(*parts):
    shape = parts[0].shape
    join = len(shape) == 3
    shape = (shape[0], len(parts) * shape[1], shape[2]) if join else (len(parts),) + shape
    return pl.pallas_call(
        functools.partial(pack_kernel, join),
        out_shape=jax.ShapeDtypeStruct(shape, parts[0].dtype),
        in_specs=[VMEM] * len(parts),
        out_specs=VMEM,
        compiler_params=pltpu.CompilerParams(vmem_limit_bytes=2 * 2**20),
        cost_estimate=pl.CostEstimate(flops=1000, bytes_accessed=0, transcendentals=0),
    )(*parts)


def half_kernel(own, out, fourth):
    q, _, _ = place()
    quarter = out.shape[1]
    for i, at in enumerate((q, q ^ 3)):
        out[i] = own[2, pl.ds(aligned(at, quarter), quarter)]
    fourth[...] = out[0]


def half_of(own):
    quarter = own.shape[1] // lax.axis_size("sp")
    return pl.pallas_call(
        half_kernel,
        out_shape=[
            jax.ShapeDtypeStruct((2, quarter, own.shape[2]), own.dtype),
            jax.ShapeDtypeStruct((quarter, own.shape[2]), own.dtype),
        ],
        in_specs=[VMEM],
        out_specs=[VMEM] * 2,
        compiler_params=pltpu.CompilerParams(vmem_limit_bytes=2 * 2**20),
        cost_estimate=pl.CostEstimate(flops=1000, bytes_accessed=0, transcendentals=0),
    )(own)


def edge_kernel(current, out):
    out[...] = current[pl.ds(current.shape[0] - HALO, HALO)]


def edge(current):
    return pl.pallas_call(
        edge_kernel,
        out_shape=jax.ShapeDtypeStruct((HALO, current.shape[1]), current.dtype),
        in_specs=[VMEM],
        out_specs=VMEM,
        compiler_params=pltpu.CompilerParams(vmem_limit_bytes=2 * 2**20),
        cost_estimate=pl.CostEstimate(flops=1000, bytes_accessed=0, transcendentals=0),
    )(current)


def own_kernel(lin, gate, proj, out, sems):
    run_copies([(w, out.at[i]) for i, w in enumerate((lin, gate, proj))], sems)


def own_shards(lin, gate, proj):
    return pl.pallas_call(
        own_kernel,
        out_shape=jax.ShapeDtypeStruct((3,) + lin.shape, lin.dtype),
        in_specs=[pl.BlockSpec(memory_space=pltpu.HBM)] * 3,
        out_specs=VMEM,
        scratch_shapes=[pltpu.SemaphoreType.DMA((3,))],
        compiler_params=pltpu.CompilerParams(vmem_limit_bytes=2 * 2**20),
        cost_estimate=pl.CostEstimate(flops=1000, bytes_accessed=0, transcendentals=0),
    )(lin, gate, proj)


def norm_kernel(current, earlier, gain, normed):
    normed[0:HALO] = rms_rows(earlier[...], gain[...])
    for row in range(0, current.shape[0], HALO):
        normed[pl.ds(HALO + row, HALO)] = rms_rows(current[pl.ds(row, HALO)], gain[...])


def norm(current, earlier, gain):
    rows, width = current.shape
    return pl.pallas_call(
        norm_kernel,
        out_shape=jax.ShapeDtypeStruct((HALO + rows, width), BF16),
        in_specs=[VMEM] * 3,
        out_specs=VMEM,
        compiler_params=pltpu.CompilerParams(vmem_limit_bytes=4 * 2**20),
        cost_estimate=pl.CostEstimate(flops=10**9, bytes_accessed=0, transcendentals=0),
    )(current, earlier, gain.reshape(1, width))


def settle(target, side, parts, q, core):
    own, first, second = parts
    quarter = second[0].shape[0] // 2
    shard = 4 * quarter
    for i in range(len(own)):

        def put(at, value):
            target[i, pl.ds(aligned(at, quarter) + side * shard, quarter), :] = value

        put(q, own[i][:quarter])
        put(q ^ (1 + core), first[i][...] if first else own[i][quarter:])
        put(q ^ (2 - core), second[i][:quarter])
        put(q ^ 3, second[i][quarter:])


def piece_kernel(turn, normed, *refs):
    q, z, c = place()
    hop = HOPS[turn]
    taps, bias, conv, mixed, weights = refs[-5:]
    rows, lanes = conv.shape
    half = lanes // 2
    if turn == 0:
        own, other = refs[:2]
        for i in range(2):
            weights[i, :half] = own[i]
            weights[i, half:] = other[i]
    else:
        own, first, second, other_two, other_second = ([r.at[0], r.at[1]] for r in refs[:5])
        settle(weights, 0, (own, first, second), q, c)
        settle(weights, 1, (other_two, None, other_second), q, 1 - c)
    hidden = normed[...]
    contract = (((1,), (1,)), ((), ()))
    linear = lax.dot_general(hidden, weights[0], contract, preferred_element_type=F32)
    gating = lax.dot_general(hidden, weights[1], contract, preferred_element_type=F32)
    gated = (linear * jax.nn.sigmoid(gating)).astype(BF16).astype(F32)
    for i in range(mixed.shape[0]):
        mixed[i] = gated[:, i * 128 : (i + 1) * 128]
    block = 64
    for side in range(2):
        shard = 2 * (z ^ hop) + (c ^ side)
        for lane in range(0, half, 128):
            cols = pl.ds(side * half + lane, 128)
            source = pl.ds(aligned(shard * (half // 128) + lane // 128, 128), 128)
            weights = taps[:, source].astype(F32)
            start = bias[0:1, source]
            for row in range(0, rows, block):
                total = jnp.broadcast_to(start, (block, 128))
                for low in range(8):
                    first = row + low + HALO - REACH
                    reach = min(block + 24, mixed.shape[1] - first)
                    window = mixed[(side * half + lane) // 128, pl.ds(first, reach), :]
                    for high in range(4):
                        tap = 8 * high + low
                        if tap < KW:
                            total += weights[tap : tap + 1] * window[8 * high : 8 * high + block]
                conv[pl.ds(row, block), cols] = total


def piece(turn, normed, weights, taps, bias, lanes):
    rows = normed.shape[0] - HALO
    flops = 4 * normed.shape[0] * normed.shape[1] * lanes
    return pl.pallas_call(
        functools.partial(piece_kernel, turn),
        out_shape=jax.ShapeDtypeStruct((rows, lanes), F32),
        in_specs=[VMEM] * (3 + len(weights)),
        out_specs=VMEM,
        scratch_shapes=[
            pltpu.VMEM((lanes // 128, normed.shape[0], 128), F32),
            pltpu.VMEM((2, lanes, normed.shape[1]), BF16),
        ],
        compiler_params=pltpu.CompilerParams(vmem_limit_bytes=6 * 2**20),
        cost_estimate=pl.CostEstimate(flops=flops, bytes_accessed=0, transcendentals=0),
    )(normed, *weights, taps, bias)


def active_kernel(current, gain, shift, own, other, *refs):
    convs, (acts, partial) = refs[:-2], refs[-2:]
    _, z, c = place()
    lanes = convs[0].shape[1]
    half = lanes // 2
    channels = len(convs) * lanes
    total = sum(jnp.sum(v[...], axis=1, keepdims=True) for v in convs)
    square = sum(jnp.sum(v[...] * v[...], axis=1, keepdims=True) for v in convs)
    mean = total / channels
    var = square / channels - mean * mean
    scale = lax.rsqrt(var + EPS)
    for i, (hop, v) in enumerate(zip(HOPS, convs)):
        for side in range(2):
            source = pl.ds(aligned(2 * (z ^ hop) + (c ^ side), half), half)
            y = (v[:, side * half : (side + 1) * half] - mean) * scale * gain[0:1, source] + shift[0:1, source]
            acts[i, :, side * half : (side + 1) * half] = (y * jax.nn.sigmoid(y)).astype(BF16)
    act = acts[0]
    partial[...] = (
        current[...].astype(F32)
        + jnp.dot(act[:, :half], own[2], preferred_element_type=F32)
        + jnp.dot(act[:, half:], other[2], preferred_element_type=F32)
    )


def active(current, gain, shift, own, other, convs):
    rows, width = current.shape
    lanes = convs[0].shape[1]
    return pl.pallas_call(
        active_kernel,
        out_shape=[
            jax.ShapeDtypeStruct((len(convs), rows, lanes), BF16),
            jax.ShapeDtypeStruct((rows, width), F32),
        ],
        in_specs=[VMEM] * (5 + len(convs)),
        out_specs=[VMEM] * 2,
        compiler_params=pltpu.CompilerParams(vmem_limit_bytes=8 * 2**20),
        cost_estimate=pl.CostEstimate(flops=4 * rows * width * lanes, bytes_accessed=0, transcendentals=0),
    )(current, gain, shift, own, other, *convs)


def finish_kernel(acts, partial, *refs):
    halves, quarters, out, whole = refs[:4], refs[4:-2], refs[-2], refs[-1]
    q, _, c = place()
    quarter = halves[0].shape[1]

    @pl.when(pl.program_id(0) == 0)
    def _():
        for side in range(2):
            step = 1 + (c ^ side)
            near, far = halves[2 * side : 2 * side + 2]
            for at, value in ((q, near[0]), (q ^ 3, near[1]), (q ^ step, far[0]), (q ^ step ^ 3, far[1])):
                whole[0, pl.ds(aligned(at, quarter) + side * 4 * quarter, quarter), :] = value
        own, first, second, other_two, other_second = ([r.at[0], r.at[1]] for r in quarters)
        settle(whole.at[1:], 0, (own, first, second), q, c)
        settle(whole.at[1:], 1, (other_two, None, other_second), q, 1 - c)

    width = out.shape[1]
    cols = pl.ds(aligned(pl.program_id(0), width), width)
    total = partial[:, cols]
    for k in range(whole.shape[0]):
        total += jnp.dot(acts[k + 1], whole[k, :, cols], preferred_element_type=F32)
    out[...] = total.astype(BF16)


def finish(acts, partial, parts):
    rows, width = partial.shape
    hops, lanes = acts.shape[0] - 1, acts.shape[2]
    step = width // 4
    return pl.pallas_call(
        finish_kernel,
        grid=(width // step,),
        out_shape=jax.ShapeDtypeStruct((rows, width), BF16),
        in_specs=[VMEM] * (2 + len(parts)),
        out_specs=pl.BlockSpec((rows, step), lambda i: (0, i)),
        scratch_shapes=[pltpu.VMEM((hops, lanes, width), BF16)],
        compiler_params=pltpu.CompilerParams(vmem_limit_bytes=6 * 2**20),
        cost_estimate=pl.CostEstimate(flops=2 * rows * width * hops * lanes, bytes_accessed=0, transcendentals=0),
    )(acts, partial, *parts)


def send(value, target):
    ways, both = lax.axis_size("sp"), lax.axis_size("tp")
    pairs = []
    for q in range(ways):
        for z in range(both // 2):
            for c in range(2):
                t = target(q, z, c)
                if t is not None:
                    pairs.append((q * both + z * 2 + c, t[0] * both + t[1] * 2 + t[2]))
    return lax.ppermute(value, ("sp", "tp"), pairs)


def plane_first(q, z, c):
    return (q ^ (1 + c), z, c)


def plane_second(q, z, c):
    return (q ^ (2 - c), z, c)


def other_core(q, z, c):
    return (q, z, 1 - c)


def along(hop):
    return lambda q, z, c: (q, z ^ hop, c)


def fast(stream, norm_gain, w_lin, w_gate, conv_taps, conv_bias, ln_gain, ln_shift, w_proj):
    current = stream[0]
    ways, lanes = lax.axis_size("sp"), 2 * w_lin.shape[0]

    quarter = w_lin.shape[0] // ways
    q, _, _ = place()

    def cut(w, at):
        return lax.dynamic_slice_in_dim(w, at * quarter, quarter, 0)

    own = own_shards(w_lin, w_gate, w_proj)
    gates = pack(cut(w_lin, q), cut(w_gate, q))
    near = send(gates, along(1))
    across = send(gates, along(3))
    opposite = send(gates, along(2))
    far = [near, across, opposite]
    half, fourth = half_of(own)
    far_half = send(half, along(1))
    far_fourths = [send(fourth, along(k)) for k in HOPS[2:]]
    tail = edge(current)
    earlier = send(tail, lambda q, z, c: (q + 1, z, c) if q + 1 < ways else None)
    other = send(own, other_core)
    normed = norm(current, earlier, norm_gain)
    bias = conv_bias.reshape(1, -1)
    convs = [piece(0, normed, [own, other], conv_taps, bias, lanes)]
    for k, mine in enumerate(far, 1):
        first = send(mine, plane_first)
        two = pack(mine, first)
        second = send(two, plane_second)
        parts = [mine, first, second, send(two, other_core), send(second, other_core)]
        convs.append(piece(k, normed, parts, conv_taps, bias, lanes))
    plane = send(far_half, plane_first)
    parts = [far_half, plane, send(far_half, other_core), send(plane, other_core)]
    mine = pack(*far_fourths)
    first = send(mine, plane_first)
    two = pack(mine, first)
    second = send(two, plane_second)
    parts += [mine, first, second, send(two, other_core), send(second, other_core)]
    acts, partial = active(current, ln_gain.reshape(1, -1), ln_shift.reshape(1, -1), own, other, convs)
    return finish(acts, partial, parts)[None]


def quick(mesh_shape, shard):
    ways, both = mesh_shape["sp"], mesh_shape["tp"]
    return ways == 4 and both == 8 and shard % (16 * ways) == 0 and shard % 128 == 0


def solution(mesh):
    shape = dict(mesh.shape)
    placed = (
        P("tp", "sp", None),
        P(),
        P("tp", None),
        P("tp", None),
        P(),
        P(),
        P(),
        P(),
        P("tp", None),
    )

    def local(*args):
        if quick(shape, args[2].shape[0]):
            return fast(*args)
        return plain(*args)

    return jax.shard_map(local, mesh=mesh, in_specs=placed, out_specs=P("tp", "sp", None), check_vma=False)
```

```python
import functools

import jax
import jax.numpy as jnp
from jax import lax
from jax.experimental import pallas as pl
from jax.experimental.pallas import tpu as pltpu
from jax.sharding import PartitionSpec as P


KW = 31
REACH = KW - 1
HALO = 32
EPS = 1e-06
F32 = jnp.float32
BF16 = jnp.bfloat16
VMEM = pl.BlockSpec(memory_space=pltpu.VMEM)


def rms_rows(rows, gain):
    full = rows.astype(F32)
    scale = lax.rsqrt(jnp.mean(full * full, axis=1, keepdims=True) + EPS)
    return (full * scale * gain).astype(BF16)


def passed_along(value, axis, steps):
    count = lax.axis_size(axis)
    leading, last = (max(0, -steps), min(count, count - steps))
    return lax.ppermute(value, axis, [(source, source + steps) for source in range(leading, last)])


def plain(stream, norm_gain, w_lin, w_gate, conv_taps, conv_bias, ln_gain, ln_shift, w_proj):
    rows = stream.shape[1]
    current = stream[0]
    normed = rms_rows(current, norm_gain)
    paired = jnp.stack([w_lin, w_gate], axis=1)
    both = jnp.einsum(
        "td,nrd->trn",
        normed,
        lax.all_gather(paired, "tp", axis=0, tiled=True),
        preferred_element_type=F32,
    )
    mixed = (both[:, 0] * jax.nn.sigmoid(both[:, 1])).astype(BF16)
    earlier_mixed = passed_along(mixed[rows - REACH :], "sp", 1)
    padded = jnp.concatenate([earlier_mixed, mixed], axis=0).astype(F32)
    taps_full = conv_taps.astype(F32)
    conv = jnp.zeros((rows, mixed.shape[1]), F32)
    for tap in range(KW):
        conv = conv + taps_full[tap] * padded[tap : tap + rows]
    conv = conv + conv_bias
    mean = jnp.mean(conv, axis=1, keepdims=True)
    meansq = jnp.mean(conv * conv, axis=1, keepdims=True)
    var = meansq - mean * mean
    activated = jax.nn.silu((conv - mean) * lax.rsqrt(var + EPS) * ln_gain + ln_shift).astype(BF16)
    projected = jnp.dot(
        activated, lax.all_gather(w_proj, "tp", axis=0, tiled=True), preferred_element_type=F32
    )
    return (current.astype(F32) + projected).astype(BF16)[None]


def place():
    me = lax.axis_index("tp")
    return lax.axis_index("sp"), me // 2, me % 2


def aligned(value, unit):
    return pl.multiple_of(value * unit, unit)


HOPS = (0, 1, 3, 2)


def run_copies(pairs, sems):
    copies = [pltpu.make_async_copy(a, b, sems.at[i]) for i, (a, b) in enumerate(pairs)]
    for copy in copies:
        copy.start()
    for copy in copies:
        copy.wait()


def pack_kernel(join, *refs):
    parts, out = refs[:-1], refs[-1]
    step = parts[0].shape[-2]
    for i, part in enumerate(parts):
        if join:
            out[:, i * step : (i + 1) * step] = part[...]
        else:
            out[i] = part[...]


def pack(*parts):
    shape = parts[0].shape
    join = len(shape) == 3
    shape = (shape[0], len(parts) * shape[1], shape[2]) if join else (len(parts),) + shape
    return pl.pallas_call(
        functools.partial(pack_kernel, join),
        out_shape=jax.ShapeDtypeStruct(shape, parts[0].dtype),
        in_specs=[VMEM] * len(parts),
        out_specs=VMEM,
        compiler_params=pltpu.CompilerParams(vmem_limit_bytes=2 * 2**20),
        cost_estimate=pl.CostEstimate(flops=1000, bytes_accessed=0, transcendentals=0),
    )(*parts)


def half_kernel(own, out, fourth):
    q, _, _ = place()
    quarter = out.shape[1]
    for i, at in enumerate((q, q ^ 3)):
        out[i] = own[2, pl.ds(aligned(at, quarter), quarter)]
    fourth[...] = out[0]


def half_of(own):
    quarter = own.shape[1] // lax.axis_size("sp")
    return pl.pallas_call(
        half_kernel,
        out_shape=[
            jax.ShapeDtypeStruct((2, quarter, own.shape[2]), own.dtype),
            jax.ShapeDtypeStruct((quarter, own.shape[2]), own.dtype),
        ],
        in_specs=[VMEM],
        out_specs=[VMEM] * 2,
        compiler_params=pltpu.CompilerParams(vmem_limit_bytes=2 * 2**20),
        cost_estimate=pl.CostEstimate(flops=1000, bytes_accessed=0, transcendentals=0),
    )(own)


def edge_kernel(current, out):
    out[...] = current[pl.ds(current.shape[0] - HALO, HALO)]


def edge(current):
    return pl.pallas_call(
        edge_kernel,
        out_shape=jax.ShapeDtypeStruct((HALO, current.shape[1]), current.dtype),
        in_specs=[VMEM],
        out_specs=VMEM,
        compiler_params=pltpu.CompilerParams(vmem_limit_bytes=2 * 2**20),
        cost_estimate=pl.CostEstimate(flops=1000, bytes_accessed=0, transcendentals=0),
    )(current)


def own_kernel(lin, gate, proj, out, sems):
    run_copies([(w, out.at[i]) for i, w in enumerate((lin, gate, proj))], sems)


def own_shards(lin, gate, proj):
    return pl.pallas_call(
        own_kernel,
        out_shape=jax.ShapeDtypeStruct((3,) + lin.shape, lin.dtype),
        in_specs=[pl.BlockSpec(memory_space=pltpu.HBM)] * 3,
        out_specs=VMEM,
        scratch_shapes=[pltpu.SemaphoreType.DMA((3,))],
        compiler_params=pltpu.CompilerParams(vmem_limit_bytes=2 * 2**20),
        cost_estimate=pl.CostEstimate(flops=1000, bytes_accessed=0, transcendentals=0),
    )(lin, gate, proj)


def norm_kernel(current, earlier, gain, normed):
    normed[0:HALO] = rms_rows(earlier[...], gain[...])
    for row in range(0, current.shape[0], HALO):
        normed[pl.ds(HALO + row, HALO)] = rms_rows(current[pl.ds(row, HALO)], gain[...])


def norm(current, earlier, gain):
    rows, width = current.shape
    return pl.pallas_call(
        norm_kernel,
        out_shape=jax.ShapeDtypeStruct((HALO + rows, width), BF16),
        in_specs=[VMEM] * 3,
        out_specs=VMEM,
        compiler_params=pltpu.CompilerParams(vmem_limit_bytes=4 * 2**20),
        cost_estimate=pl.CostEstimate(flops=10**9, bytes_accessed=0, transcendentals=0),
    )(current, earlier, gain.reshape(1, width))


def settle(target, side, parts, q, core):
    own, first, second = parts
    quarter = second[0].shape[0] // 2
    shard = 4 * quarter
    for i in range(len(own)):

        def put(at, value):
            target[i, pl.ds(aligned(at, quarter) + side * shard, quarter), :] = value

        put(q, own[i][:quarter])
        put(q ^ (1 + core), first[i][...] if first else own[i][quarter:])
        put(q ^ (2 - core), second[i][:quarter])
        put(q ^ 3, second[i][quarter:])


def piece_kernel(turn, normed, *refs):
    q, z, c = place()
    hop = HOPS[turn]
    taps, bias, conv, mixed, weights = refs[-5:]
    rows, lanes = conv.shape
    half = lanes // 2
    if turn == 0:
        own, other = refs[:2]
        for i in range(2):
            weights[i, :half] = own[i]
            weights[i, half:] = other[i]
    else:
        own, first, second, other_two, other_second = ([r.at[0], r.at[1]] for r in refs[:5])
        settle(weights, 0, (own, first, second), q, c)
        settle(weights, 1, (other_two, None, other_second), q, 1 - c)
    hidden = normed[...]
    contract = (((1,), (1,)), ((), ()))
    linear = lax.dot_general(hidden, weights[0], contract, preferred_element_type=F32)
    gating = lax.dot_general(hidden, weights[1], contract, preferred_element_type=F32)
    gated = (linear * jax.nn.sigmoid(gating)).astype(BF16).astype(F32)
    for i in range(mixed.shape[0]):
        mixed[i] = gated[:, i * 128 : (i + 1) * 128]
    block = 64
    for side in range(2):
        shard = 2 * (z ^ hop) + (c ^ side)
        for lane in range(0, half, 128):
            cols = pl.ds(side * half + lane, 128)
            source = pl.ds(aligned(shard * (half // 128) + lane // 128, 128), 128)
            weights = taps[:, source].astype(F32)
            start = bias[0:1, source]
            for row in range(0, rows, block):
                total = jnp.broadcast_to(start, (block, 128))
                for low in range(8):
                    first = row + low + HALO - REACH
                    reach = min(block + 24, mixed.shape[1] - first)
                    window = mixed[(side * half + lane) // 128, pl.ds(first, reach), :]
                    for high in range(4):
                        tap = 8 * high + low
                        if tap < KW:
                            total += weights[tap : tap + 1] * window[8 * high : 8 * high + block]
                conv[pl.ds(row, block), cols] = total


def piece(turn, normed, weights, taps, bias, lanes):
    rows = normed.shape[0] - HALO
    flops = 4 * normed.shape[0] * normed.shape[1] * lanes
    return pl.pallas_call(
        functools.partial(piece_kernel, turn),
        out_shape=jax.ShapeDtypeStruct((rows, lanes), F32),
        in_specs=[VMEM] * (3 + len(weights)),
        out_specs=VMEM,
        scratch_shapes=[
            pltpu.VMEM((lanes // 128, normed.shape[0], 128), F32),
            pltpu.VMEM((2, lanes, normed.shape[1]), BF16),
        ],
        compiler_params=pltpu.CompilerParams(vmem_limit_bytes=6 * 2**20),
        cost_estimate=pl.CostEstimate(flops=flops, bytes_accessed=0, transcendentals=0),
    )(normed, *weights, taps, bias)


def active_kernel(current, gain, shift, own, other, *refs):
    convs, (acts, partial) = refs[:-2], refs[-2:]
    _, z, c = place()
    lanes = convs[0].shape[1]
    half = lanes // 2
    channels = len(convs) * lanes
    total = sum(jnp.sum(v[...], axis=1, keepdims=True) for v in convs)
    square = sum(jnp.sum(v[...] * v[...], axis=1, keepdims=True) for v in convs)
    mean = total / channels
    var = square / channels - mean * mean
    scale = lax.rsqrt(var + EPS)
    for i, (hop, v) in enumerate(zip(HOPS, convs)):
        for side in range(2):
            source = pl.ds(aligned(2 * (z ^ hop) + (c ^ side), half), half)
            y = (v[:, side * half : (side + 1) * half] - mean) * scale * gain[0:1, source] + shift[0:1, source]
            acts[i, :, side * half : (side + 1) * half] = (y * jax.nn.sigmoid(y)).astype(BF16)
    act = acts[0]
    partial[...] = (
        current[...].astype(F32)
        + jnp.dot(act[:, :half], own[2], preferred_element_type=F32)
        + jnp.dot(act[:, half:], other[2], preferred_element_type=F32)
    )


def active(current, gain, shift, own, other, convs):
    rows, width = current.shape
    lanes = convs[0].shape[1]
    return pl.pallas_call(
        active_kernel,
        out_shape=[
            jax.ShapeDtypeStruct((len(convs), rows, lanes), BF16),
            jax.ShapeDtypeStruct((rows, width), F32),
        ],
        in_specs=[VMEM] * (5 + len(convs)),
        out_specs=[VMEM] * 2,
        compiler_params=pltpu.CompilerParams(vmem_limit_bytes=8 * 2**20),
        cost_estimate=pl.CostEstimate(flops=4 * rows * width * lanes, bytes_accessed=0, transcendentals=0),
    )(current, gain, shift, own, other, *convs)


CHUNKS = 4


def column_chunks(width):
    step = width // CHUNKS
    return [pl.ds(i * step, step) for i in range(CHUNKS)]


def gather_kernel(acts, partial, *refs):
    halves, quarters, out, whole = refs[:4], refs[4:-2], refs[-2], refs[-1]
    q, _, c = place()
    quarter = halves[0].shape[1]
    for side in range(2):
        step = 1 + (c ^ side)
        near, far = halves[2 * side : 2 * side + 2]
        for at, value in ((q, near[0]), (q ^ 3, near[1]), (q ^ step, far[0]), (q ^ step ^ 3, far[1])):
            whole[0, pl.ds(aligned(at, quarter) + side * 4 * quarter, quarter), :] = value
    own, first, second, other_two = ([r.at[0], r.at[1]] for r in quarters)
    nothing = [jnp.zeros((2 * quarter, whole.shape[2]), BF16)] * len(own)
    settle(whole.at[1:], 0, (own, first, second), q, c)
    settle(whole.at[1:], 1, (other_two, None, nothing), q, 1 - c)
    for cols in column_chunks(out.shape[1]):
        total = partial[:, cols]
        for k in range(whole.shape[0]):
            total += jnp.dot(acts[k + 1], whole[k, :, cols], preferred_element_type=F32)
        out[:, cols] = total


def gather(acts, partial, parts):
    rows, width = partial.shape
    hops, lanes = acts.shape[0] - 1, acts.shape[2]
    return pl.pallas_call(
        gather_kernel,
        out_shape=jax.ShapeDtypeStruct((rows, width), F32),
        in_specs=[VMEM] * (2 + len(parts)),
        out_specs=VMEM,
        scratch_shapes=[pltpu.VMEM((hops, lanes, width), BF16)],
        compiler_params=pltpu.CompilerParams(vmem_limit_bytes=8 * 2**20),
        cost_estimate=pl.CostEstimate(flops=2 * rows * width * hops * lanes, bytes_accessed=0, transcendentals=0),
    )(acts, partial, *parts)


def finish_kernel(acts, partial, last, out, whole, ready, sems):
    q, _, c = place()
    pieces, quarter = last.shape[0], last.shape[1] // 2
    half = whole.shape[1]
    core = 1 - c
    whole[...] = jnp.zeros_like(whole)
    for k in range(pieces):
        for i, at in enumerate((q ^ (2 - core), q ^ 3)):
            whole[k, pl.ds(aligned(at, quarter), quarter), :] = last[k, i * quarter : (i + 1) * quarter]
    copies = []
    for i, cols in enumerate(column_chunks(out.shape[1])):
        total = partial[:, cols]
        for k in range(pieces):
            act = acts[acts.shape[0] - pieces + k, :, half:]
            total += jnp.dot(act, whole[k, :, cols], preferred_element_type=F32)
        ready[:, cols] = total.astype(BF16)
        copies.append(pltpu.make_async_copy(ready.at[:, cols], out.at[:, cols], sems.at[i]))
        copies[-1].start()
    for copy in copies:
        copy.wait()


def finish(acts, partial, last):
    rows, width = partial.shape
    pieces, half = last.shape[0], acts.shape[2] // 2
    return pl.pallas_call(
        finish_kernel,
        out_shape=jax.ShapeDtypeStruct((rows, width), BF16),
        in_specs=[VMEM] * 3,
        out_specs=pl.BlockSpec(memory_space=pltpu.HBM),
        scratch_shapes=[
            pltpu.VMEM((pieces, half, width), BF16),
            pltpu.VMEM((rows, width), BF16),
            pltpu.SemaphoreType.DMA((CHUNKS,)),
        ],
        compiler_params=pltpu.CompilerParams(vmem_limit_bytes=8 * 2**20),
        cost_estimate=pl.CostEstimate(flops=2 * rows * width * pieces * half, bytes_accessed=0, transcendentals=0),
    )(acts, partial, last)


def send(value, target):
    ways, both = lax.axis_size("sp"), lax.axis_size("tp")
    pairs = []
    for q in range(ways):
        for z in range(both // 2):
            for c in range(2):
                t = target(q, z, c)
                if t is not None:
                    pairs.append((q * both + z * 2 + c, t[0] * both + t[1] * 2 + t[2]))
    return lax.ppermute(value, ("sp", "tp"), pairs)


def plane_first(q, z, c):
    return (q ^ (1 + c), z, c)


def plane_second(q, z, c):
    return (q ^ (2 - c), z, c)


def other_core(q, z, c):
    return (q, z, 1 - c)


def along(hop):
    return lambda q, z, c: (q, z ^ hop, c)


def fast(stream, norm_gain, w_lin, w_gate, conv_taps, conv_bias, ln_gain, ln_shift, w_proj):
    current = stream[0]
    ways, lanes = lax.axis_size("sp"), 2 * w_lin.shape[0]

    quarter = w_lin.shape[0] // ways
    q, _, _ = place()

    def cut(w, at):
        return lax.dynamic_slice_in_dim(w, at * quarter, quarter, 0)

    own = own_shards(w_lin, w_gate, w_proj)
    gates = pack(cut(w_lin, q), cut(w_gate, q))
    near = send(gates, along(1))
    across = send(gates, along(3))
    opposite = send(gates, along(2))
    far = [near, across, opposite]
    half, fourth = half_of(own)
    far_half = send(half, along(1))
    far_fourths = [send(fourth, along(k)) for k in HOPS[2:]]
    tail = edge(current)
    earlier = send(tail, lambda q, z, c: (q + 1, z, c) if q + 1 < ways else None)
    other = send(own, other_core)
    normed = norm(current, earlier, norm_gain)
    bias = conv_bias.reshape(1, -1)
    convs = [piece(0, normed, [own, other], conv_taps, bias, lanes)]
    for k, mine in enumerate(far, 1):
        first = send(mine, plane_first)
        two = pack(mine, first)
        second = send(two, plane_second)
        parts = [mine, first, second, send(two, other_core), send(second, other_core)]
        convs.append(piece(k, normed, parts, conv_taps, bias, lanes))
    plane = send(far_half, plane_first)
    parts = [far_half, plane, send(far_half, other_core), send(plane, other_core)]
    mine = pack(*far_fourths)
    first = send(mine, plane_first)
    two = pack(mine, first)
    second = send(two, plane_second)
    parts += [mine, first, second, send(two, other_core)]
    last = send(second, other_core)
    acts, partial = active(current, ln_gain.reshape(1, -1), ln_shift.reshape(1, -1), own, other, convs)
    partial = gather(acts, partial, parts)
    return finish(acts, partial, last)[None]


def quick(mesh_shape, shard):
    ways, both = mesh_shape["sp"], mesh_shape["tp"]
    return ways == 4 and both == 8 and shard % (16 * ways) == 0 and shard % 128 == 0


def solution(mesh):
    shape = dict(mesh.shape)
    placed = (
        P("tp", "sp", None),
        P(),
        P("tp", None),
        P("tp", None),
        P(),
        P(),
        P(),
        P(),
        P("tp", None),
    )

    def local(*args):
        if quick(shape, args[2].shape[0]):
            return fast(*args)
        return plain(*args)

    return jax.shard_map(local, mesh=mesh, in_specs=placed, out_specs=P("tp", "sp", None), check_vma=False)
```
